32 devices in a mesh: ep: 4 (over y, x), tp: 8 (over z, core).
Axes of the slice: x: 2, y: 2, z: 4, core: 2. Of those that a mesh axis runs over, the one named last changes fastest.
Arguments:
- tokens: bfloat16 [64, 4096], P('ep'), may hold values from -6 to 6
- query_weight: bfloat16 [4096, 4096], P('ep', 'tp'), may hold values from -0.09375 to 0.09375
- key_weight: bfloat16 [4096, 2048], P('ep', 'tp'), may hold values from -0.15625 to 0.15625
- value_weight: bfloat16 [4096, 2048], P('ep', 'tp'), may hold values from -0.09375 to 0.09375
- out_weight: bfloat16 [4096, 4096], P('tp', 'ep'), may hold values from -0.09375 to 0.09375
- head_lambda: float32 [32], P('tp'), may hold values from 0.3 to 0.8
- head_gain: float32 [128], replicated, may hold values from 0.1 to 1.9
- key_cache: bfloat16 [64, 1024, 16, 128], P('ep', None, 'tp'), may hold values from -1000 to 1000
- value_cache: bfloat16 [64, 1024, 16, 128], P('ep', None, 'tp'), may hold values from -6 to 6
- lengths: int32 [64], P('ep'), may hold values from 128 to 1024, as said below
- first_gain: float32 [4096], replicated, may hold values from 0.3 to 3
- second_gain: float32 [4096], P('tp'), may hold values from 0.1 to 1.9
- expert_ids: int32 [64, 2], P('ep'), may hold values from 0 to 15, all different within a row; in each aligned block of 16 rows (0 to 15, 16 to 31, ...) at most 4 rows name the same one
- route_weights: float32 [64, 2], P('ep'), may hold values from 0.1 to 1
- expert_gate: bfloat16 [16, 4096, 2048], P('ep', 'tp'), may hold values from -0.09375 to 0.09375
- expert_up: bfloat16 [16, 4096, 2048], P('ep', 'tp'), may hold values from -0.09375 to 0.09375
- expert_down: bfloat16 [16, 2048, 4096], P('ep', None, 'tp'), may hold values from -0.125 to 0.125
- dense_gate: bfloat16 [4096, 2048], P('tp', 'ep'), may hold values from -0.09375 to 0.09375
- dense_up: bfloat16 [4096, 2048], P('tp', 'ep'), may hold values from -0.09375 to 0.09375
- dense_down: bfloat16 [2048, 4096], P('ep', 'tp'), may hold values from -0.25 to 0.25
- dense_mix: bfloat16 [4096], replicated, may hold values from -0.09375 to 0.09375
Outputs:
- layer_out: bfloat16 [64, 4096], P('ep', 'tp')
The draws below stay inside these ranges and needn't reach their ends.
Inputs may be any that keep to these rules, and one draw needn't show every extreme that they name: `lengths`: positions below a sequence's length hold its cache; the new token stands at that position. Some sequence has length 1024 in every draw. `expert_ids`: each row names 2 different experts. Among the rows of one device's 16 sequences (aligned blocks) no expert is named more than 4 times, and in every draw some expert is named exactly 4 times in some block.
All inputs are finite; a program needn't handle non-finite values.
Results may differ from the reference program's by a relative error of at most 0.04.
Values may be sent and summed in bfloat16 or wider, within the bound.
A program may use at most 128 MiB of HBM per device.

```python
import math
import jax
import jax.numpy as jnp
import numpy as np
from jax import lax

D = 4096
HEADS = 32
KV_HEADS = 16
SUB = 64
VD = 128
EXPERTS = 16
FFE = 2048
FFD = 2048
TOPK = 2
SEQ_DEV = 16
CACHE = 1024
SEQS = 64
CAP = 4


def draw_key_cache(key, part):
    rand_keys = jax.random.split(jax.random.fold_in(key, 11), 1)
    full_shape = (SEQS, CACHE, KV_HEADS, 2 * SUB)
    values = jnp.clip(1.75 * jax.random.normal(rand_keys[0], full_shape, jnp.float32), -10.5, 10.5)
    return values.astype(jnp.bfloat16)


def draw_lengths(key, part):
    rand_keys = jax.random.split(jax.random.fold_in(key, 23), 3)
    group_rate = jax.random.randint(rand_keys[0], (SEQS // SEQ_DEV,), 1, 5)
    seq_rate = jnp.repeat(group_rate, SEQ_DEV)
    shortest = CACHE // 8
    raw_draw = jax.random.randint(rand_keys[1], (SEQS,), 0, CACHE)
    lengths = shortest + raw_draw * seq_rate * (CACHE - shortest) // (4 * CACHE)
    longest = jax.random.randint(rand_keys[2], (), 0, SEQS)
    return jnp.where(jnp.arange(SEQS, dtype=jnp.int32) == longest, CACHE, lengths).astype(jnp.int32)


def draw_first_gain(key, part):
    rand_keys = jax.random.split(jax.random.fold_in(key, 37), 2)
    ramp = jnp.arange(D, dtype=jnp.float32) / (D - 1)
    trend = jnp.exp(jnp.log(0.5) + ramp * (jnp.log(2.0) - jnp.log(0.5)))
    rough = jax.random.uniform(rand_keys[1], (D,), jnp.float32, 0.7, 1.4)
    return (trend * rough).astype(jnp.float32)


def steps_of(key, dims, cuts, least, top_value):
    factor_of = 1.0
    for dim, parts in cuts:
        steps = jax.random.uniform(jax.random.fold_in(jax.random.fold_in(key, 6), dim), (parts,), jnp.float32, least / len(cuts), top_value / len(cuts))
        factor_of = factor_of * jnp.repeat(jnp.exp(steps), dims[dim] // parts).reshape((-1,) + (1,) * (len(dims) - 1 - dim))
    return factor_of


def assign_block(own_key, own, number, rows, count, top, limit, skew):
    ranking = jax.random.permutation(own_key, count)
    heavy_load, usual = portions_of(count, rows * top, limit, skew, True), portions_of(count, rows * top, limit, skew, False)
    places = jnp.arange(count)

    def named(sizes, rotation):
        used = int((sizes > 0).sum())
        fixed = max(1, used // 4)
        passed = fixed + (places - fixed + rotation * (used - fixed)) % max(1, count - fixed)
        return jnp.zeros((count,), jnp.int32).at[ranking[jnp.where(places < fixed, places, passed)]].set(jnp.asarray(sizes, jnp.int32))

    sizes = jnp.where(number % 4 == 0, named(heavy_load, number // 4), named(usual, number - number // 4 - 1))
    mixed = jax.random.permutation(jax.random.fold_in(own, 3), count)
    giver, sink = mixed[0:count // 2 * 2:2], mixed[1:count // 2 * 2:2]
    slack = jnp.minimum(sizes[giver] - 1, limit - sizes[sink]) // 2
    slack = jnp.where((giver == ranking[0]) | (sink == ranking[0]) | (sizes[sink] == 0), 0, jnp.maximum(slack, 0))
    passed = jax.random.randint(jax.random.fold_in(own, 4), (count // 2,), 0, 1 << 20) % (slack + 1)
    sizes = sizes.at[giver].add(-passed).at[sink].add(passed)
    items = jnp.searchsorted(jnp.cumsum(sizes), jnp.arange(rows * top), side="right").astype(jnp.int32)
    table = items.reshape(top, rows).T
    table = table[jax.random.permutation(jax.random.fold_in(own, 1), rows)]
    rotation = jax.random.randint(jax.random.fold_in(own, 2), (rows, 1), 0, top)
    return jnp.take_along_axis(table, (jnp.arange(top)[None, :] + rotation) % top, axis=1)


def portions_of(amount, total, bound, lean, full):
    portions = [(1 << 20) // math.isqrt(rank ** lean) + 1 for rank in range(1, amount + 1)]
    largest = bound if full else min(bound, max(-(-total // amount), total * portions[0] // sum(portions)))
    least = 1 if total - largest >= amount - 1 else 0
    given, rest = [largest] + [least] * (amount - 1), total - largest - least * (amount - 1)
    while rest > 0:
        movable = [i for i in range(1, amount) if given[i] < largest] or [i for i in range(1, amount) if given[i] < bound]
        mass, left = sum([portions[i] for i in movable]), rest
        for i in movable:
            addition = min(bound - given[i], max(1, left * portions[i] // mass), rest)
            given[i] = given[i] + addition
            rest = rest - addition
    return np.array(given)


def centred(rng, shape, scale, bound, cuts=(), kind=jnp.bfloat16):
    drawn = scale * jax.random.normal(rng, shape, jnp.float32)
    if cuts:
        drawn = drawn * steps_of(rng, shape, cuts, -0.22, 0.18)
    return jnp.clip(drawn, -bound, bound).astype(kind)


def setup_inputs(seed: int = 0) -> dict:
    splits = jax.random.split(jax.random.key(seed), 22)
    tokens = centred(splits[0], (SEQS, D), 1.0, 6.0, ((0, 4),))
    query_weight = centred(splits[1], (D, HEADS * 2 * SUB), D ** -0.5, 0.09375, ((0, 4), (1, 8)))
    key_weight = centred(splits[2], (D, KV_HEADS * 2 * SUB), (D // 3) ** -0.5, 0.15625, ((0, 4), (1, 8)))
    value_weight = centred(splits[3], (D, KV_HEADS * VD), D ** -0.5, 0.09375, ((0, 4), (1, 8)))
    out_weight = centred(splits[4], (HEADS * VD, D), (HEADS * VD) ** -0.5, 0.09375, ((0, 8), (1, 4)))
    head_lambda = jnp.clip(0.3 + 0.5 * jax.random.uniform(splits[5], (HEADS,), jnp.float32) ** steps_of(splits[5], (HEADS,), ((0, 8),), -0.2, 0.2), 0.3, 0.8)
    head_gain = jnp.clip(1.0 + 0.18 * jax.random.normal(splits[6], (VD,), jnp.float32), 0.1, 1.9)
    key_cache = draw_key_cache(jax.random.fold_in(splits[21], 71), 0)
    value_cache = centred(splits[8], (SEQS, CACHE, KV_HEADS, VD), 1.0, 6.0, ((0, 4), (2, 8)))
    lengths = draw_lengths(jax.random.fold_in(splits[21], 71), 0)
    first_gain = draw_first_gain(jax.random.fold_in(splits[21], 71), 0)
    second_gain = jnp.clip(1.0 + 0.18 * jax.random.normal(splits[11], (D,), jnp.float32), 0.1, 1.9)
    expert_ids_keys = jax.random.split(jax.random.fold_in(splits[12], 1), SEQS // SEQ_DEV)
    expert_ids_turns = jax.random.permutation(jax.random.fold_in(splits[12], 3), SEQS // SEQ_DEV)
    expert_ids = jax.vmap(lambda own, number: assign_block(jax.random.fold_in(splits[12], 2), own, number, SEQ_DEV, EXPERTS, TOPK, CAP, 2))(expert_ids_keys, expert_ids_turns).reshape((SEQS, TOPK))
    route_weights = jnp.clip(jnp.exp(math.log(1.0) - 2.3025851 * jax.random.uniform(splits[13], (SEQS, TOPK), jnp.float32) ** steps_of(splits[13], (SEQS, TOPK), ((0, 4),), -0.2, 0.2)), 0.1, 1.0)
    expert_gate = centred(splits[14], (EXPERTS, D, FFE), D ** -0.5, 0.09375, ((0, 4), (1, 8)))
    expert_up = centred(splits[15], (EXPERTS, D, FFE), D ** -0.5, 0.09375, ((0, 4), (1, 8)))
    expert_down = centred(splits[16], (EXPERTS, FFE, D), FFE ** -0.5, 0.125, ((0, 4), (2, 8)))
    dense_gate = centred(splits[17], (D, FFD), D ** -0.5, 0.09375, ((0, 8), (1, 4)))
    dense_up = centred(splits[18], (D, FFD), D ** -0.5, 0.09375, ((0, 8), (1, 4)))
    dense_down = centred(splits[19], (FFD, D), (FFD // 4) ** -0.5, 0.25, ((0, 4), (1, 8)))
    dense_mix = centred(splits[20], (D,), D ** -0.5, 0.09375)
    return dict(tokens=tokens, query_weight=query_weight, key_weight=key_weight, value_weight=value_weight, out_weight=out_weight, head_lambda=head_lambda, head_gain=head_gain, key_cache=key_cache, value_cache=value_cache, lengths=lengths, first_gain=first_gain, second_gain=second_gain, expert_ids=expert_ids, route_weights=route_weights, expert_gate=expert_gate, expert_up=expert_up, expert_down=expert_down, dense_gate=dense_gate, dense_up=dense_up, dense_down=dense_down, dense_mix=dense_mix)


theta_base = 500000.0
score_scale = 0.125
head_scale = 0.8
residual_scale = 2.0 ** 0.5
layer_epsilon = 1e-05
head_epsilon = 1e-06

def rotate(vector, cosine, sine_table):
    middle = vector.shape[-1] // 2
    lower = vector[..., :middle]
    upper = vector[..., middle:]
    return jnp.concatenate([lower * cosine - upper * sine_table, upper * cosine + lower * sine_table], axis=-1)

def rounded(array):
    return lax.optimization_barrier(array.astype(jnp.bfloat16)).astype(jnp.float32)

def reference(tokens, query_weight, key_weight, value_weight, out_weight, head_lambda, head_gain, key_cache, value_cache, lengths, first_gain, second_gain, expert_ids, route_weights, expert_gate, expert_up, expert_down, dense_gate, dense_up, dense_down, dense_mix):
    group_size = HEADS // KV_HEADS
    frequency = theta_base ** (-(jnp.arange(SUB // 2, dtype=jnp.float32) * (2.0 / SUB)))
    angles = lengths.astype(jnp.float32)[:, None] * frequency[None, :]
    cosine = jnp.cos(angles)
    sine_table = jnp.sin(angles)
    query_rows = rounded(jnp.dot(tokens, query_weight, preferred_element_type=jnp.float32))
    query_rows = query_rows.reshape(SEQS, KV_HEADS, group_size, 2, SUB)
    query_rows = rounded(rotate(query_rows, cosine[:, None, None, None, :], sine_table[:, None, None, None, :]))
    new_keys = rounded(jnp.dot(tokens, key_weight, preferred_element_type=jnp.float32))
    new_keys = rounded(rotate(new_keys.reshape(SEQS, KV_HEADS, 2, SUB), cosine[:, None, None, :], sine_table[:, None, None, :]))
    new_values = rounded(jnp.dot(tokens, value_weight, preferred_element_type=jnp.float32))
    new_values = new_values.reshape(SEQS, KV_HEADS, VD)
    lambdas = head_lambda.reshape(KV_HEADS, group_size)
    valid = jnp.arange(CACHE, dtype=jnp.int32)[None, :] < lengths[:, None]

    def head_step(head):
        cached_keys = lax.dynamic_index_in_dim(key_cache, head, 2, keepdims=False).astype(jnp.float32)
        cached_keys = cached_keys.reshape(SEQS, CACHE, 2, SUB)
        cached_values = lax.dynamic_index_in_dim(value_cache, head, 2, keepdims=False).astype(jnp.float32)
        head_query = lax.dynamic_index_in_dim(query_rows, head, 1, keepdims=False)
        head_key = lax.dynamic_index_in_dim(new_keys, head, 1, keepdims=False)
        head_value = lax.dynamic_index_in_dim(new_values, head, 1, keepdims=False)
        pair = lax.dynamic_index_in_dim(lambdas, head, 0, keepdims=False)
        scores = jnp.einsum('sgcd,sjcd->sgcj', head_query, cached_keys) * score_scale
        scores = jnp.where(valid[:, None, None, :], scores, -jnp.inf)
        fresh_score = jnp.einsum('sgcd,scd->sgc', head_query, head_key) * score_scale
        highest = jnp.maximum(lax.optimization_barrier(jnp.max(scores, axis=-1)), fresh_score)
        cached_exp = jnp.exp(scores - highest[..., None])
        fresh_exp = jnp.exp(fresh_score - highest)
        denominator = lax.optimization_barrier(jnp.sum(cached_exp, axis=-1)) + fresh_exp
        cached_prob = cached_exp / denominator[..., None]
        fresh_prob = fresh_exp / denominator
        mixed_map = rounded(cached_prob[:, :, 0] - pair[None, :, None] * cached_prob[:, :, 1])
        mixed_new = rounded(fresh_prob[:, :, 0] - pair[None, :] * fresh_prob[:, :, 1])
        return jnp.einsum('sgj,sje->sge', mixed_map, cached_values) + mixed_new[..., None] * head_value[:, None, :]
    head_out = lax.map(head_step, jnp.arange(KV_HEADS, dtype=jnp.int32))
    head_out = jnp.moveaxis(head_out, 0, 1)
    square_mean = lax.optimization_barrier(jnp.mean(head_out * head_out, axis=-1, keepdims=True))
    normed = head_out * lax.rsqrt(square_mean + head_epsilon) * head_gain * head_scale
    normed = normed.astype(jnp.bfloat16).reshape(SEQS, HEADS * VD)
    attention = rounded(jnp.dot(normed, out_weight, preferred_element_type=jnp.float32))
    residual_in = residual_scale * tokens.astype(jnp.float32) + attention
    average = lax.optimization_barrier(jnp.mean(residual_in, axis=-1, keepdims=True))
    centered = residual_in - average
    variance = lax.optimization_barrier(jnp.mean(centered * centered, axis=-1, keepdims=True))
    hidden_in = (centered * lax.rsqrt(variance + layer_epsilon) * first_gain).astype(jnp.bfloat16)
    route_gates = route_weights / lax.optimization_barrier(jnp.sum(route_weights, axis=-1, keepdims=True))

    def expert_step(running, expert):
        gate_matrix = lax.dynamic_index_in_dim(expert_gate, expert, 0, keepdims=False)
        up_matrix = lax.dynamic_index_in_dim(expert_up, expert, 0, keepdims=False)
        down_matrix = lax.dynamic_index_in_dim(expert_down, expert, 0, keepdims=False)
        pre_gate = jnp.dot(hidden_in, gate_matrix, preferred_element_type=jnp.float32)
        pre_up = jnp.dot(hidden_in, up_matrix, preferred_element_type=jnp.float32)
        expert_hidden = (jax.nn.silu(pre_gate) * pre_up).astype(jnp.bfloat16)
        expert_result = rounded(jnp.dot(expert_hidden, down_matrix, preferred_element_type=jnp.float32))
        token_weight = lax.optimization_barrier(jnp.sum(jnp.where(expert_ids == expert, route_gates, 0.0), axis=-1))
        return (running + token_weight[:, None] * expert_result, None)
    expert_mix, _ = lax.scan(expert_step, jnp.zeros((SEQS, D), jnp.float32), jnp.arange(EXPERTS, dtype=jnp.int32))
    dense_pre_gate = jnp.dot(hidden_in, dense_gate, preferred_element_type=jnp.float32)
    dense_pre_up = jnp.dot(hidden_in, dense_up, preferred_element_type=jnp.float32)
    dense_hidden = (jax.nn.silu(dense_pre_gate) * dense_pre_up).astype(jnp.bfloat16)
    dense_out = rounded(jnp.dot(dense_hidden, dense_down, preferred_element_type=jnp.float32))
    mix_gate = jax.nn.sigmoid(jnp.dot(hidden_in, dense_mix, preferred_element_type=jnp.float32))
    combined = residual_scale * hidden_in.astype(jnp.float32) + expert_mix + mix_gate[:, None] * dense_out
    average = lax.optimization_barrier(jnp.mean(combined, axis=-1, keepdims=True))
    variance = lax.optimization_barrier(jnp.mean(combined * combined, axis=-1, keepdims=True)) - average * average
    return ((combined - average) * lax.rsqrt(variance + layer_epsilon) * second_gain).astype(jnp.bfloat16)
```

```python
import functools

import jax
import jax.numpy as jnp
from jax import lax
from jax.experimental import pallas as pl
from jax.experimental.pallas import tpu as pltpu
from jax.sharding import PartitionSpec as P

SUB = 64
EXPERTS = 16
TOPK = 2
CAP = 4
PAD = 16
LANES = 128

theta_base = 500000.0
score_scale = 0.125
head_scale = 0.8
residual_scale = 2.0**0.5
layer_epsilon = 1e-05
head_epsilon = 1e-06
F32 = jnp.float32
BF16 = jnp.bfloat16
MESH = pl.DeviceIdType.MESH


def mm(a, b):
    return lax.dot_general(a, b, (((1,), (0,)), ((), ())), preferred_element_type=F32)


def aligned(index, size):
    return pl.ds(pl.multiple_of(index * size, LANES), size)


def kernel(
    ep, tp, kv, heads,
    tok, cosr, sinr, lens, lam, hgain, fgain, sgain, ids, rw, dmix,
    qw, kw, vw, ow, kc, vc, eg, eu, ed, dg, du, dd,
    out,
    wq, wk, wv, wo, kbuf, vbuf, weg, weu, wed, wdg, wdu, wdd,
    cols, sB, rB, qs, ks, vs, hn, heads_all, sD, rD, stat, mixp, sE, rE, arr,
    sF, rF, sFd, rFd, hG, hGd, acc, sH, rH, mom,
    wsem, ksem, vsem, esem, ssem, rsem, sdsem, rdsem,
):
    me = lax.axis_index("ep")
    mt = lax.axis_index("tp")
    seqs = tok.shape[0]
    cdim = qw.shape[0]
    qc, kcn = qw.shape[1], kw.shape[1]
    own = ed.shape[2]
    width = tok.shape[1]
    ratio = tp // ep
    le = eg.shape[0]
    slots = ep * CAP
    fc = eg.shape[2] // tp
    fd = dg.shape[1]
    nrow = 2 * heads

    def load(src, dst, sem):
        cp = pltpu.make_async_copy(src, dst, sem)
        cp.start()
        return cp

    cq = load(qw, wq, wsem.at[0])
    ck = load(kw, wk, wsem.at[1])
    cv = load(vw, wv, wsem.at[2])

    sends = []

    def post(phase, axis, src, dst):
        n, mine = (ep, me) if axis == "ep" else (tp, mt)
        copies = []
        for k in range(1, n):
            peer = lax.rem(mine + k, n)
            where = (peer, mt) if axis == "ep" else (me, peer)
            cp = pltpu.make_async_remote_copy(
                src_ref=src(peer), dst_ref=dst(mine),
                send_sem=ssem.at[phase, k], recv_sem=rsem.at[phase, k],
                device_id=where, device_id_type=MESH,
            )
            cp.start()
            copies.append(cp)
        sends.extend(copies)
        return copies

    def arrive(copies):
        for cp in copies:
            cp.wait_recv()

    got = post(0, "ep", lambda p: tok.at[:, aligned(p, cdim)], lambda m: cols.at[m])
    cols[me] = tok[:, aligned(me, cdim)]

    kcp = [load(kc.at[s], kbuf.at[s], ksem.at[s]) for s in range(seqs)]
    vcp = [load(vc.at[s], vbuf.at[s], vsem.at[s]) for s in range(seqs)]
    co = load(ow, wo, wsem.at[3])
    cdg = load(dg, wdg, wsem.at[4])
    cdu = load(du, wdu, wsem.at[5])
    cdd = load(dd, wdd, wsem.at[6])
    ecp = []
    for e in range(le):
        ecp.append(load(eg.at[e], weg.at[e], esem.at[0, e]))
        ecp.append(load(eu.at[e], weu.at[e], esem.at[1, e]))
    edc = [load(ed.at[e], wed.at[e], esem.at[2, e]) for e in range(le)]

    lane = lax.broadcasted_iota(jnp.int32, (seqs, LANES), 1)
    idv = [ids[:, k : k + 1] for k in range(TOPK)]
    hit = [(lane == i).astype(F32) for i in idv]
    low = (
        lax.broadcasted_iota(jnp.int32, (seqs, seqs), 1)
        < lax.broadcasted_iota(jnp.int32, (seqs, seqs), 0)
    ).astype(BF16)
    earlier = mm(low, (hit[0] + hit[1]).astype(BF16))
    rsum = rw[:, 0:1] + rw[:, 1:2]
    slot_lane = lax.broadcasted_iota(jnp.int32, (seqs, ep * PAD), 1)
    place = jnp.zeros((seqs, ep * PAD), F32)
    mixw = jnp.zeros((seqs, ep * PAD), F32)
    for k in range(TOPK):
        slot = jnp.sum(earlier * hit[k], axis=1, keepdims=True).astype(jnp.int32)
        home = jnp.zeros_like(idv[k])
        for p in range(1, ep):
            home = home + (idv[k] >= p * le).astype(jnp.int32)
        col = home * PAD + (idv[k] - home * le) * CAP + slot
        eq = (slot_lane == col).astype(F32)
        place = place + eq
        mixw = mixw + eq * (rw[:, k : k + 1] / rsum)

    cq.wait()
    ck.wait()
    cv.wait()
    arrive(got)
    x = cols[...].reshape(ep * seqs, cdim)
    sB[:, :, 0:qc] = mm(x, wq[...]).astype(BF16).reshape(ep, seqs, qc)
    sB[:, :, qc : qc + kcn] = mm(x, wk[...]).astype(BF16).reshape(ep, seqs, kcn)
    sB[:, :, qc + kcn :] = mm(x, wv[...]).astype(BF16).reshape(ep, seqs, kcn)
    got = post(1, "ep", lambda p: sB.at[p], lambda m: rB.at[m])
    rB[me] = sB[me]
    arrive(got)
    total = rB[0].astype(F32)
    for p in range(1, ep):
        total = total + rB[p].astype(F32)
    total = total.astype(BF16).astype(F32)

    lane = lax.broadcasted_iota(jnp.int32, (seqs, LANES), 1)
    lower = (lane & (SUB - 1)) < SUB // 2
    first = lane < SUB
    cosine, sine = cosr[...], sinr[...]

    def turned(v):
        up = pltpu.roll(v, LANES - SUB // 2, 1)
        down = pltpu.roll(v, SUB // 2, 1)
        return (v * cosine + jnp.where(lower, up, down) * sine).astype(BF16).astype(F32)

    group = heads // kv
    for k in range(kv):
        krot = turned(total[:, qc + k * LANES : qc + (k + 1) * LANES])
        vnew = total[:, qc + kcn + k * LANES : qc + kcn + (k + 1) * LANES]
        for g in range(group):
            h = k * group + g
            q = turned(total[:, h * LANES : (h + 1) * LANES])
            qs[:, h, :] = jnp.where(first, q, 0.0)
            qs[:, heads + h, :] = jnp.where(first, 0.0, q)
            ks[:, h, :] = krot
            ks[:, heads + h, :] = krot
            vs[:, h, :] = vnew

    npos = kbuf.shape[1]
    ccol = lax.broadcasted_iota(jnp.int32, (nrow, npos), 1)
    crow = lax.broadcasted_iota(jnp.int32, (nrow, npos), 0)
    krow = jnp.zeros_like(crow)
    for r in range(nrow):
        krow = jnp.where(crow == r, (r % heads) // group, krow)
    mine = lax.rem(ccol, kv) == krow if kv > 1 else ccol >= 0
    lamc = lam[...]
    gain = hgain[...] * head_scale

    def one(s):
        q8 = qs[s]
        score = lax.dot_general(
            q8.astype(BF16), kbuf[s], (((1,), (1,)), ((), ())), preferred_element_type=F32
        )
        score = jnp.where(mine & (ccol < lens[s] * kv), score * score_scale, -1e30)
        fresh = jnp.sum(q8 * ks[s], axis=1, keepdims=True) * score_scale
        high = jnp.maximum(jnp.max(score, axis=1, keepdims=True), fresh)
        ex = jnp.exp(score - high)
        fx = jnp.exp(fresh - high)
        inv = 1.0 / (jnp.sum(ex, axis=1, keepdims=True) + fx)
        pr = ex * inv
        fp = fx * inv
        dmap = (pr[0:heads] - lamc * pr[heads:nrow]).astype(BF16)
        dnew = (fp[0:heads] - lamc * fp[heads:nrow]).astype(BF16).astype(F32)
        ho = mm(dmap, vbuf[s]) + dnew * vs[s]
        sq = jnp.mean(ho * ho, axis=1, keepdims=True)
        hn[s] = ho * lax.rsqrt(sq + head_epsilon) * gain

    step = 4

    def some(i, carry):
        for u in range(step):
            s = i * step + u
            pltpu.make_async_copy(kc.at[s], kbuf.at[s], ksem.at[s]).wait()
            pltpu.make_async_copy(vc.at[s], vbuf.at[s], vsem.at[s]).wait()
        for u in range(step):
            one(i * step + u)
        return carry

    lax.fori_loop(0, seqs // step, some, 0)
    for h in range(heads):
        heads_all[me, :, h * LANES : (h + 1) * LANES] = hn[:, h, :].astype(BF16)
    got = post(2, "ep", lambda p: heads_all.at[me], lambda m: heads_all.at[m])
    co.wait()
    arrive(got)
    part = mm(heads_all[...].reshape(ep * seqs, heads * LANES), wo[...])
    for h in range(ratio):
        sD[h] = part[:, h * own : (h + 1) * own].astype(BF16).reshape(ep, seqs, own)

    def dcopy(ds, h):
        s = lax.rem(me + ds, ep)
        t = me * ratio + h
        return t, pltpu.make_async_remote_copy(
            src_ref=sD.at[h, s], dst_ref=rD.at[mt],
            send_sem=sdsem.at[ds, h], recv_sem=rdsem.at[mt],
            device_id=(s, t), device_id_type=MESH,
        )

    for ds in range(ep):
        for h in range(ratio):
            t, cp = dcopy(ds, h)
            if ds == 0:
                @pl.when(t == mt)
                def _():
                    pltpu.make_async_copy(sD.at[h, me], rD.at[mt], rdsem.at[mt]).start()

                @pl.when(t != mt)
                def _():
                    cp.start()
            else:
                cp.start()
    for t in range(tp):
        pltpu.make_async_copy(rD.at[t], rD.at[t], rdsem.at[t]).wait()
    attn = rD[0].astype(F32)
    for t in range(1, tp):
        attn = attn + rD[t].astype(F32)
    attn = attn.astype(BF16).astype(F32)
    resid = residual_scale * tok[:, aligned(mt, own)].astype(F32) + attn
    mloc = jnp.mean(resid, axis=1, keepdims=True)
    cent = resid - mloc
    m2 = jnp.sum(cent * cent, axis=1, keepdims=True)
    stat[mt] = jnp.where(lane == 0, mloc, m2)
    got = post(3, "tp", lambda p: stat.at[mt], lambda m: stat.at[m])
    arrive(got)
    mean = stat[0]
    for t in range(1, tp):
        mean = mean + stat[t]
    sqs = mean[:, 1:2]
    mean = mean[:, 0:1] * (1.0 / tp)
    for t in range(tp):
        d = stat[t][:, 0:1] - mean
        sqs = sqs + d * d * own
    rstd = lax.rsqrt(sqs * (1.0 / width) + layer_epsilon)
    hidden = ((resid - mean) * rstd * fgain[:, aligned(mt, own)]).astype(BF16)
    hidf = hidden.astype(F32)
    dotp = jnp.sum(hidf * dmix[:, aligned(mt, own)], axis=1, keepdims=True)

    packed = lax.dot_general(
        place, hidf, (((0,), (0,)), ((), ())), preferred_element_type=F32
    ).astype(BF16)
    for p in range(ep):
        sE[p, 0:seqs] = hidden
        sE[p, seqs : seqs + PAD] = packed[p * PAD : (p + 1) * PAD]
    got = post(4, "ep", lambda p: sE.at[p], lambda m: rE.at[m])
    mixp[mt] = jnp.broadcast_to(dotp, (seqs, LANES))
    got_mix = post(5, "tp", lambda p: mixp.at[mt], lambda m: mixp.at[m])
    rE[me] = sE[me]
    nslot = le * slots
    prow = lax.broadcasted_iota(jnp.int32, (nslot, ep * PAD), 0)
    pcol = lax.broadcasted_iota(jnp.int32, (nslot, ep * PAD), 1)
    pe, ps, pc = prow // slots, (prow % slots) // CAP, prow % CAP
    perm = (pcol == ps * PAD + pe * CAP + pc).astype(BF16)
    arrive(got)
    rows = rE[:, 0:seqs].reshape(ep * seqs, own)
    routed = rE[:, seqs : seqs + PAD].reshape(ep * PAD, own)
    arr[...] = mm(perm, routed).astype(BF16)

    cdg.wait()
    cdu.wait()
    sFd[:, :, 0:fd] = mm(rows, wdg[...]).reshape(tp, ep * seqs // tp, fd).astype(BF16)
    sFd[:, :, fd:] = mm(rows, wdu[...]).reshape(tp, ep * seqs // tp, fd).astype(BF16)
    got_d = post(6, "tp", lambda p: sFd.at[p], lambda m: rFd.at[m])
    rFd[mt] = sFd[mt]
    for cp in ecp:
        cp.wait()

    def fcopy(k):
        peer = lax.rem(mt + k, tp)
        return pltpu.make_async_remote_copy(
            src_ref=sF.at[peer], dst_ref=rF.at[mt],
            send_sem=ssem.at[7, k], recv_sem=rsem.at[7, k],
            device_id=(me, peer), device_id_type=MESH,
        )

    def chunk(peer, into):
        for e in range(le):
            xe = arr[e * slots : (e + 1) * slots]
            into[peer, 0, e * slots : (e + 1) * slots] = mm(
                xe, weg[e, :, aligned(peer, fc)]
            ).astype(BF16)
            into[peer, 1, e * slots : (e + 1) * slots] = mm(
                xe, weu[e, :, aligned(peer, fc)]
            ).astype(BF16)

    def fstep(k, carry):
        chunk(lax.rem(mt + k, tp), sF)
        fcopy(k).start()
        return carry

    lax.fori_loop(1, tp, fstep, 0)
    chunk(mt, rF)

    arrive(got_d)
    dsum = rFd[0].astype(F32)
    for t in range(1, tp):
        dsum = dsum + rFd[t].astype(F32)
    dg_, du_ = dsum[:, 0:fd], dsum[:, fd:]
    hGd[mt] = (dg_ / (1.0 + jnp.exp(-dg_)) * du_).astype(BF16)
    got_d = post(8, "tp", lambda p: hGd.at[mt], lambda m: hGd.at[m])

    for k in range(1, tp):
        fcopy(k).wait_recv()
    gs, us = rF[0, 0].astype(F32), rF[0, 1].astype(F32)
    for t in range(1, tp):
        gs = gs + rF[t, 0].astype(F32)
        us = us + rF[t, 1].astype(F32)
    hG[mt] = (gs / (1.0 + jnp.exp(-gs)) * us).astype(BF16)
    got = post(9, "tp", lambda p: hG.at[mt], lambda m: hG.at[m])

    cdd.wait()
    arrive(got_d)
    dh = hGd[...].astype(F32).reshape(ep * seqs, fd).astype(BF16)
    sH[:, PAD : PAD + seqs] = mm(dh, wdd[...]).astype(BF16).reshape(ep, seqs, own)
    for cp in edc:
        cp.wait()

    def down(src):
        for e in range(le):
            acc[e] += mm(hG[src, e * slots : (e + 1) * slots], wed[e, aligned(src, fc), :])

    acc[...] = jnp.zeros_like(acc)
    down(mt)
    for k in range(1, tp):
        got[k - 1].wait_recv()
        down(lax.rem(mt + tp - k, tp))
    res = acc[...].reshape(nslot, own).astype(BF16)
    back = lax.dot_general(
        perm, res, (((0,), (0,)), ((), ())), preferred_element_type=F32
    ).astype(BF16)
    sH[:, 0:PAD] = back.reshape(ep, PAD, own)
    got = post(10, "ep", lambda p: sH.at[p], lambda m: rH.at[m])
    rH[me] = sH[me]
    arrive(got_mix)
    mixs = mixp[0]
    for t in range(1, tp):
        mixs = mixs + mixp[t]
    gate = 1.0 / (1.0 + jnp.exp(-mixs[:, 0:1]))
    arrive(got)
    returned = rH[:, 0:PAD].reshape(ep * PAD, own)
    hi = mixw.astype(BF16)
    rest = mixw - hi.astype(F32)
    mid = rest.astype(BF16)
    last = (rest - mid.astype(F32)).astype(BF16)
    emix = mm(hi, returned) + mm(mid, returned) + mm(last, returned)
    dout = rH[0, PAD : PAD + seqs].astype(F32)
    for p in range(1, ep):
        dout = dout + rH[p, PAD : PAD + seqs].astype(F32)
    dout = dout.astype(BF16).astype(F32)
    comb = residual_scale * hidf + emix + gate * dout
    s1 = jnp.sum(comb, axis=1, keepdims=True)
    s2 = jnp.sum(comb * comb, axis=1, keepdims=True)
    mom[mt] = jnp.where(lane == 0, s1, s2)
    got = post(11, "tp", lambda p: mom.at[mt], lambda m: mom.at[m])
    arrive(got)
    ms = mom[0]
    for t in range(1, tp):
        ms = ms + mom[t]
    ms = ms * (1.0 / width)
    avg = ms[:, 0:1]
    var = ms[:, 1:2] - avg * avg
    out[...] = ((comb - avg) * lax.rsqrt(var + layer_epsilon) * sgain[...]).astype(BF16)

    for cp in sends:
        cp.wait_send()
    for k in range(1, tp):
        fcopy(k).wait_send()
    for ds in range(ep):
        for h in range(ratio):
            t, cp = dcopy(ds, h)
            if ds == 0:
                @pl.when(t != mt)
                def _():
                    cp.wait_send()
            else:
                cp.wait_send()


PHASES = 12


def on_device(
    tokens, query_weight, key_weight, value_weight, out_weight, head_lambda, head_gain,
    key_cache, value_cache, lengths, first_gain, second_gain, expert_ids, route_weights,
    expert_gate, expert_up, expert_down, dense_gate, dense_up, dense_down, dense_mix,
):
    ep, tp = lax.axis_size("ep"), lax.axis_size("tp")
    seqs, width = tokens.shape
    cache, kv, vd = key_cache.shape[1:]
    heads = head_lambda.shape[0]
    cdim, qc = query_weight.shape
    kcn = key_weight.shape[1]
    le, own, ffe = expert_gate.shape
    fd = dense_gate.shape[1]
    fc = ffe // tp
    ratio = tp // ep
    slots = ep * CAP
    rows = ep * seqs
    npos = cache * kv
    lanes = jnp.arange(LANES, dtype=jnp.int32)
    half = SUB // 2
    frequency = theta_base ** (-((lanes % half).astype(F32) * (2.0 / SUB)))
    angles = lengths.astype(F32)[:, None] * frequency[None, :]
    sign = jnp.where(lanes % SUB < half, -1.0, 1.0)
    cosine = jnp.cos(angles)
    sine = jnp.sin(angles) * sign[None, :]
    vm = pl.BlockSpec(memory_space=pltpu.VMEM)
    sm = pl.BlockSpec(memory_space=pltpu.SMEM)
    hb = pl.BlockSpec(memory_space=pl.ANY)
    V = pltpu.VMEM
    D = pltpu.SemaphoreType.DMA
    n = max(ep, tp)
    return pl.pallas_call(
        functools.partial(kernel, ep, tp, kv, heads),
        out_shape=jax.ShapeDtypeStruct((seqs, own), BF16),
        in_specs=[vm] * 3 + [sm] + [vm] * 7 + [hb] * 12,
        out_specs=vm,
        scratch_shapes=[
            V(query_weight.shape, BF16), V(key_weight.shape, BF16), V(value_weight.shape, BF16),
            V(out_weight.shape, BF16),
            V((seqs, npos, vd), BF16), V((seqs, npos, vd), BF16),
            V(expert_gate.shape, BF16), V(expert_up.shape, BF16), V(expert_down.shape, BF16),
            V(dense_gate.shape, BF16), V(dense_up.shape, BF16), V(dense_down.shape, BF16),
            V((ep, seqs, cdim), BF16),
            V((ep, seqs, qc + 2 * kcn), BF16), V((ep, seqs, qc + 2 * kcn), BF16),
            V((seqs, 2 * heads, LANES), F32), V((seqs, 2 * heads, LANES), F32),
            V((seqs, heads, LANES), F32), V((seqs, heads, LANES), F32),
            V((ep, seqs, heads * LANES), BF16),
            V((ratio, ep, seqs, own), BF16), V((tp, seqs, own), BF16),
            V((tp, seqs, LANES), F32), V((tp, seqs, LANES), F32),
            V((ep, seqs + PAD, own), BF16), V((ep, seqs + PAD, own), BF16),
            V((le * slots, own), BF16),
            V((tp, 2, le * slots, fc), BF16), V((tp, 2, le * slots, fc), BF16),
            V((tp, rows // tp, 2 * fd), BF16), V((tp, rows // tp, 2 * fd), BF16),
            V((tp, le * slots, fc), BF16), V((tp, rows // tp, fd), BF16),
            V((le, slots, own), F32),
            V((ep, PAD + seqs, own), BF16), V((ep, PAD + seqs, own), BF16),
            V((tp, seqs, LANES), F32),
            D((7,)), D((seqs,)), D((seqs,)), D((3, le)),
            D((PHASES, n)), D((PHASES, n)), D((ep, ratio)), D((tp,)),
        ],
        compiler_params=pltpu.CompilerParams(
            has_side_effects=True, vmem_limit_bytes=62 * 1024 * 1024
        ),
        name="layer",
    )(
        tokens, cosine, sine, lengths, head_lambda.reshape(heads, 1), head_gain.reshape(1, -1),
        first_gain.reshape(1, -1), second_gain.reshape(1, -1), expert_ids, route_weights,
        dense_mix.astype(F32).reshape(1, -1),
        query_weight, key_weight, value_weight, out_weight,
        key_cache.reshape(seqs, npos, vd), value_cache.reshape(seqs, npos, vd),
        expert_gate, expert_up, expert_down, dense_gate, dense_up, dense_down,
    )


def solution(mesh):
    return jax.shard_map(
        on_device,
        mesh=mesh,
        in_specs=(
            P("ep", None), P("ep", "tp"), P("ep", "tp"), P("ep", "tp"), P("tp", "ep"),
            P("tp"), P(), P("ep", None, "tp", None), P("ep", None, "tp", None), P("ep"),
            P(), P("tp"), P("ep", None), P("ep", None), P("ep", "tp", None),
            P("ep", "tp", None), P("ep", None, "tp"), P("tp", "ep"), P("tp", "ep"),
            P("ep", "tp"), P(),
        ),
        out_specs=P("ep", "tp"),
        check_vma=False,
    )
```

```python
import functools
import math

import jax
import jax.numpy as jnp
from jax import lax
from jax.experimental import pallas as pl
from jax.experimental.pallas import tpu as pltpu
from jax.sharding import PartitionSpec as P

SUB = 64
EXPERTS = 16
TOPK = 2
CAP = 4
PAD = 16
LANES = 128

theta_base = 500000.0
score_scale = 0.125
head_scale = 0.8
residual_scale = 2.0**0.5
layer_epsilon = 1e-05
head_epsilon = 1e-06
F32 = jnp.float32
BF16 = jnp.bfloat16
MESH = pl.DeviceIdType.MESH


def mm(a, b):
    return lax.dot_general(a, b, (((1,), (0,)), ((), ())), preferred_element_type=F32)


def aligned(index, size):
    return pl.ds(pl.multiple_of(index * size, LANES), size)


def kernel(
    ep, tp, kv, heads,
    tok, lens, lam, hgain, fgain, sgain, ids, rw, dmix,
    qw, kw, vw, ow, kc, vc, eg, eu, ed, dg, du, dd,
    out,
    wq, wk, wv, wo, kbuf, vbuf, weg, weu, wed, wdg, wdu, wdd,
    cols, sB, rB, qs, ks, vs, hn, heads_all, sD, rD, stat, mixp, sE, rE, arr,
    sF, rP, sQ, rF, sFd, rPd, sQd, rFd, hG, hGd, acc, sH, rH, mom,
    wsem, ksem, vsem, esem, ssem, rsem, sdsem, rdsem, psem, qsem,
):
    me = lax.axis_index("ep")
    mt = lax.axis_index("tp")
    seqs = tok.shape[0]
    cdim = qw.shape[0]
    qc, kcn = qw.shape[1], kw.shape[1]
    own = ed.shape[2]
    width = tok.shape[1]
    ratio = tp // ep
    le = eg.shape[0]
    slots = ep * CAP
    fc = eg.shape[2] // tp
    fd = dg.shape[1]
    nrow = 2 * heads
    nz = tp // 2
    core = lax.rem(mt, 2)
    mz = lax.div(mt, 2)
    sib = mz * 2 + 1 - core

    barrier = pltpu.get_barrier_semaphore()

    def greet(e, t):
        pl.semaphore_signal(barrier, inc=1, device_id=(e, t), device_id_type=MESH)

    for k in range(1, ep):
        greet(lax.rem(me + k, ep), mt)
    for k in range(1, tp):
        greet(me, lax.rem(mt + k, tp))
    home_e = lax.div(mt, ratio)
    for s in range(ep):
        for h in range(ratio):
            t = me * ratio + h

            @pl.when((me != s) | (mt != t))
            def _():
                greet(s, t)

    for t in range(tp):

        @pl.when((me != home_e) | (mt != t))
        def _():
            greet(home_e, t)

    twice = jnp.where(home_e == me, 2 * tp - 2, 2 * tp)

    def load(src, dst, sem):
        cp = pltpu.make_async_copy(src, dst, sem)
        cp.start()
        return cp

    cq = load(qw, wq, wsem.at[0])
    ck = load(kw, wk, wsem.at[1])
    cv = load(vw, wv, wsem.at[2])
    pl.semaphore_wait(barrier, ep - 1 + tp - 1 + twice)

    sends = []

    def post(phase, axis, src, dst):
        n, mine = (ep, me) if axis == "ep" else (tp, mt)
        copies = []
        for k in range(1, n):
            peer = lax.rem(mine + k, n)
            where = (peer, mt) if axis == "ep" else (me, peer)
            cp = pltpu.make_async_remote_copy(
                src_ref=src(peer), dst_ref=dst(mine),
                send_sem=ssem.at[phase, k], recv_sem=rsem.at[phase, k],
                device_id=where, device_id_type=MESH,
            )
            cp.start()
            copies.append(cp)
        sends.extend(copies)
        return copies

    def arrive(copies):
        for cp in copies:
            cp.wait_recv()

    got = post(0, "ep", lambda p: tok.at[:, aligned(p, cdim)], lambda m: cols.at[m])
    cols[me] = tok[:, aligned(me, cdim)]

    kcp = [load(kc.at[s], kbuf.at[s], ksem.at[s]) for s in range(seqs)]
    vcp = [load(vc.at[s], vbuf.at[s], vsem.at[s]) for s in range(seqs)]
    co = load(ow, wo, wsem.at[3])
    cdg = load(dg, wdg, wsem.at[4])
    cdu = load(du, wdu, wsem.at[5])
    cdd = load(dd, wdd, wsem.at[6])
    ecp = []
    for e in range(le):
        ecp.append(load(eg.at[e], weg.at[e], esem.at[0, e]))
        ecp.append(load(eu.at[e], weu.at[e], esem.at[1, e]))
    edc = [load(ed.at[e], wed.at[e], esem.at[2, e]) for e in range(le)]

    lane = lax.broadcasted_iota(jnp.int32, (seqs, LANES), 1)
    diag = lax.broadcasted_iota(jnp.int32, (seqs, seqs), 0) == lax.broadcasted_iota(
        jnp.int32, (seqs, seqs), 1
    )

    def upright(row):
        return jnp.sum(jnp.where(diag, row[:, 0:seqs], 0.0), axis=1, keepdims=True)

    def flat(column):
        wide = lax.broadcasted_iota(jnp.int32, (seqs, LANES), 0) == lane
        return jnp.sum(jnp.where(wide, column, 0.0), axis=0, keepdims=True)

    idv = [upright(ids[k : k + 1, :].astype(F32)).astype(jnp.int32) for k in range(TOPK)]
    rwv = [upright(rw[k : k + 1, :]) for k in range(TOPK)]
    hit = [(lane == i).astype(F32) for i in idv]
    low = (
        lax.broadcasted_iota(jnp.int32, (seqs, seqs), 1)
        < lax.broadcasted_iota(jnp.int32, (seqs, seqs), 0)
    ).astype(BF16)
    earlier = mm(low, (hit[0] + hit[1]).astype(BF16))
    rsum = rwv[0] + rwv[1]
    slot_lane = lax.broadcasted_iota(jnp.int32, (seqs, ep * PAD), 1)
    place = jnp.zeros((seqs, ep * PAD), F32)
    mixw = jnp.zeros((seqs, ep * PAD), F32)
    for k in range(TOPK):
        slot = jnp.sum(earlier * hit[k], axis=1, keepdims=True).astype(jnp.int32)
        home = jnp.zeros_like(idv[k])
        for p in range(1, ep):
            home = home + (idv[k] >= p * le).astype(jnp.int32)
        col = home * PAD + (idv[k] - home * le) * CAP + slot
        eq = (slot_lane == col).astype(F32)
        place = place + eq
        mixw = mixw + eq * (rwv[k] / rsum)

    half = SUB // 2
    srow = lax.broadcasted_iota(jnp.int32, (seqs, 1), 0)
    lenc = jnp.zeros((seqs, 1), F32)
    for s in range(seqs):
        lenc = jnp.where(srow == s, lens[s].astype(F32), lenc)
    frequency = jnp.exp((lane & (half - 1)).astype(F32) * (-math.log(theta_base) / half))
    angles = lenc * frequency
    cosine = jnp.cos(angles)
    sine = jnp.where((lane & (SUB - 1)) < half, -1.0, 1.0) * jnp.sin(angles)
    lamc = jnp.zeros((heads, 1), F32)
    for h in range(heads):
        hrow = lax.broadcasted_iota(jnp.int32, (heads, 1), 0)
        lamc = jnp.where(hrow == h, lam[h], lamc)

    cq.wait()
    ck.wait()
    cv.wait()
    arrive(got)
    x = cols[...].reshape(ep * seqs, cdim)
    sB[:, :, 0:qc] = mm(x, wq[...]).astype(BF16).reshape(ep, seqs, qc)
    sB[:, :, qc : qc + kcn] = mm(x, wk[...]).astype(BF16).reshape(ep, seqs, kcn)
    sB[:, :, qc + kcn :] = mm(x, wv[...]).astype(BF16).reshape(ep, seqs, kcn)
    got = post(1, "ep", lambda p: sB.at[p], lambda m: rB.at[m])
    rB[me] = sB[me]
    arrive(got)
    total = rB[0].astype(F32)
    for p in range(1, ep):
        total = total + rB[p].astype(F32)
    total = total.astype(BF16).astype(F32)

    lane = lax.broadcasted_iota(jnp.int32, (seqs, LANES), 1)
    lower = (lane & (SUB - 1)) < SUB // 2
    first = lane < SUB

    def turned(v):
        up = pltpu.roll(v, LANES - SUB // 2, 1)
        down = pltpu.roll(v, SUB // 2, 1)
        return (v * cosine + jnp.where(lower, up, down) * sine).astype(BF16).astype(F32)

    group = heads // kv
    for k in range(kv):
        krot = turned(total[:, qc + k * LANES : qc + (k + 1) * LANES])
        vnew = total[:, qc + kcn + k * LANES : qc + kcn + (k + 1) * LANES]
        for g in range(group):
            h = k * group + g
            q = turned(total[:, h * LANES : (h + 1) * LANES])
            qs[:, h, :] = jnp.where(first, q, 0.0)
            qs[:, heads + h, :] = jnp.where(first, 0.0, q)
            ks[:, h, :] = krot
            ks[:, heads + h, :] = krot
            vs[:, h, :] = vnew

    npos = kbuf.shape[1]
    ccol = lax.broadcasted_iota(jnp.int32, (nrow, npos), 1)
    crow = lax.broadcasted_iota(jnp.int32, (nrow, npos), 0)
    krow = jnp.zeros_like(crow)
    for r in range(nrow):
        krow = jnp.where(crow == r, (r % heads) // group, krow)
    mine = lax.rem(ccol, kv) == krow if kv > 1 else ccol >= 0
    gain = hgain[...] * head_scale

    def one(s):
        q8 = qs[s]
        score = lax.dot_general(
            q8.astype(BF16), kbuf[s], (((1,), (1,)), ((), ())), preferred_element_type=F32
        )
        score = jnp.where(mine & (ccol < lens[s] * kv), score * score_scale, -1e30)
        fresh = jnp.sum(q8 * ks[s], axis=1, keepdims=True) * score_scale
        high = jnp.maximum(jnp.max(score, axis=1, keepdims=True), fresh)
        ex = jnp.exp(score - high)
        fx = jnp.exp(fresh - high)
        inv = 1.0 / (jnp.sum(ex, axis=1, keepdims=True) + fx)
        pr = ex * inv
        fp = fx * inv
        dmap = (pr[0:heads] - lamc * pr[heads:nrow]).astype(BF16)
        dnew = (fp[0:heads] - lamc * fp[heads:nrow]).astype(BF16).astype(F32)
        ho = mm(dmap, vbuf[s]) + dnew * vs[s]
        sq = jnp.mean(ho * ho, axis=1, keepdims=True)
        hn[s] = ho * lax.rsqrt(sq + head_epsilon) * gain

    step = 4

    def some(i, carry):
        for u in range(step):
            s = i * step + u
            pltpu.make_async_copy(kc.at[s], kbuf.at[s], ksem.at[s]).wait()
            pltpu.make_async_copy(vc.at[s], vbuf.at[s], vsem.at[s]).wait()
        for u in range(step):
            one(i * step + u)
        return carry

    lax.fori_loop(0, seqs // step, some, 0)
    for h in range(heads):
        heads_all[me, :, h * LANES : (h + 1) * LANES] = hn[:, h, :].astype(BF16)
    got = post(2, "ep", lambda p: heads_all.at[me], lambda m: heads_all.at[m])
    co.wait()
    arrive(got)
    part = mm(heads_all[...].reshape(ep * seqs, heads * LANES), wo[...])
    for h in range(ratio):
        sD[h] = part[:, h * own : (h + 1) * own].astype(BF16).reshape(ep, seqs, own)

    def dcopy(ds, h):
        s = lax.rem(me + ds, ep)
        t = me * ratio + h
        return t, pltpu.make_async_remote_copy(
            src_ref=sD.at[h, s], dst_ref=rD.at[mt],
            send_sem=sdsem.at[ds, h], recv_sem=rdsem.at[mt],
            device_id=(s, t), device_id_type=MESH,
        )

    for ds in range(ep):
        for h in range(ratio):
            t, cp = dcopy(ds, h)
            if ds == 0:
                @pl.when(t == mt)
                def _():
                    pltpu.make_async_copy(sD.at[h, me], rD.at[mt], rdsem.at[mt]).start()

                @pl.when(t != mt)
                def _():
                    cp.start()
            else:
                cp.start()
    for t in range(tp):
        pltpu.make_async_copy(rD.at[t], rD.at[t], rdsem.at[t]).wait()
    attn = rD[0].astype(F32)
    for t in range(1, tp):
        attn = attn + rD[t].astype(F32)
    attn = attn.astype(BF16).astype(F32)
    resid = residual_scale * tok[:, aligned(mt, own)].astype(F32) + attn
    mloc = jnp.mean(resid, axis=1, keepdims=True)
    cent = resid - mloc
    m2 = jnp.sum(cent * cent, axis=1, keepdims=True)
    stat[mt, 0:1] = flat(mloc)
    stat[mt, 1:2] = flat(m2)
    got = post(3, "tp", lambda p: stat.at[mt], lambda m: stat.at[m])
    arrive(got)
    mean = stat[0, 0:1]
    sqs = stat[0, 1:2]
    for t in range(1, tp):
        mean = mean + stat[t, 0:1]
        sqs = sqs + stat[t, 1:2]
    mean = mean * (1.0 / tp)
    for t in range(tp):
        d = stat[t, 0:1] - mean
        sqs = sqs + d * d * own
    mean, sqs = upright(mean), upright(sqs)
    rstd = lax.rsqrt(sqs * (1.0 / width) + layer_epsilon)
    hidden = ((resid - mean) * rstd * fgain[:, aligned(mt, own)]).astype(BF16)
    hidf = hidden.astype(F32)
    dmat = dmix[...].astype(F32)
    drow = lax.broadcasted_iota(jnp.int32, dmat.shape, 0)
    dotw = jnp.zeros((seqs, LANES), F32)
    for c in range(own // LANES):
        pick = jnp.sum(
            jnp.where(drow == mt * (own // LANES) + c, dmat, 0.0), axis=0, keepdims=True
        )
        dotw = dotw + hidf[:, c * LANES : (c + 1) * LANES] * pick
    dotp = jnp.sum(dotw, axis=1, keepdims=True)

    packed = lax.dot_general(
        place, hidf, (((0,), (0,)), ((), ())), preferred_element_type=F32
    ).astype(BF16)
    for p in range(ep):
        sE[p, 0:seqs] = hidden
        sE[p, seqs : seqs + PAD] = packed[p * PAD : (p + 1) * PAD]
    got = post(4, "ep", lambda p: sE.at[p], lambda m: rE.at[m])
    mixp[mt, 0:1] = flat(dotp)
    mixp[mt, 1:2] = flat(dotp)
    got_mix = post(5, "tp", lambda p: mixp.at[mt], lambda m: mixp.at[m])
    rE[me] = sE[me]
    nslot = le * slots
    prow = lax.broadcasted_iota(jnp.int32, (nslot, ep * PAD), 0)
    pcol = lax.broadcasted_iota(jnp.int32, (nslot, ep * PAD), 1)
    pe, ps, pc = prow // slots, (prow % slots) // CAP, prow % CAP
    perm = (pcol == ps * PAD + pe * CAP + pc).astype(BF16)
    arrive(got)
    rows = rE[:, 0:seqs].reshape(ep * seqs, own)
    routed = rE[:, seqs : seqs + PAD].reshape(ep * PAD, own)
    arr[...] = mm(perm, routed).astype(BF16)

    cdg.wait()
    cdu.wait()
    sFd[:, :, 0:fd] = mm(rows, wdg[...]).reshape(tp, ep * seqs // tp, fd).astype(BF16)
    sFd[:, :, fd:] = mm(rows, wdu[...]).reshape(tp, ep * seqs // tp, fd).astype(BF16)
    def pair(src, dst, kind, k):
        return pltpu.make_async_remote_copy(
            src_ref=src, dst_ref=dst,
            send_sem=psem.at[0, kind, k], recv_sem=psem.at[1, kind, k],
            device_id=(me, sib), device_id_type=MESH,
        )

    def along(src, dst, kind, k):
        return pltpu.make_async_remote_copy(
            src_ref=src, dst_ref=dst,
            send_sem=qsem.at[0, kind, k], recv_sem=qsem.at[1, kind, k],
            device_id=(me, lax.rem(mz + k, nz) * 2 + core), device_id_type=MESH,
        )

    def zof(k):
        return lax.rem(mz + k, nz)

    order = list(range(1, nz)) + [0]
    dpair = [
        pair(sFd.at[zof(k) * 2 + 1 - core], rPd.at[k], 0, k) for k in range(nz)
    ]
    for k in order:
        dpair[k].start()
    for cp in ecp:
        cp.wait()

    def chunk(peer, into, k):
        for e in range(le):
            xe = arr[e * slots : (e + 1) * slots]
            into[k, 0, e * slots : (e + 1) * slots] = mm(
                xe, weg[e, :, aligned(peer, fc)]
            ).astype(BF16)
            into[k, 1, e * slots : (e + 1) * slots] = mm(
                xe, weu[e, :, aligned(peer, fc)]
            ).astype(BF16)

    epair = [pair(sF.at[k], rP.at[k], 1, k) for k in range(nz)]
    ealong = [along(sQ.at[k], rF.at[mz], 1, k) for k in range(nz)]
    dalong = [along(sQd.at[k], rFd.at[mz], 0, k) for k in range(nz)]

    def pass_on(k):
        epair[k].wait_recv()
        if k:
            for j in range(2):
                sQ[k, j] = (sQ[k, j].astype(F32) + rP[k, j].astype(F32)).astype(BF16)
            ealong[k].start()
        else:
            for j in range(2):
                rF[mz, j] = (sQ[k, j].astype(F32) + rP[k, j].astype(F32)).astype(BF16)

    for i, k in enumerate(order):
        z = zof(k)
        chunk(z * 2 + 1 - core, sF, k)
        epair[k].start()
        chunk(z * 2 + core, sQ, k)
        dpair[k].wait_recv()
        dboth = (sFd[z * 2 + core].astype(F32) + rPd[k].astype(F32)).astype(BF16)
        if k:
            sQd[k] = dboth
            dalong[k].start()
        else:
            rFd[mz] = dboth
        if i:
            pass_on(order[i - 1])
    pass_on(order[-1])

    for k in range(1, nz):
        dalong[k].wait_recv()
    dsum = rFd[0].astype(F32)
    for t in range(1, nz):
        dsum = dsum + rFd[t].astype(F32)
    dg_, du_ = dsum[:, 0:fd], dsum[:, fd:]
    hGd[mt] = (dg_ / (1.0 + jnp.exp(-dg_)) * du_).astype(BF16)

    def spread(buf, kind):
        ways = [along(buf.at[mt], buf.at[mt], kind, k) for k in range(nz)]
        for k in range(1, nz):
            ways[k].start()
        hops = []
        for k in range(nz):
            z = lax.rem(mz + nz - k, nz) * 2
            hops.append(pair(buf.at[z + core], buf.at[z + core], kind, k))
        hops[0].start()
        return ways, hops

    dways, dhops = spread(hGd, 2)

    for k in range(1, nz):
        ealong[k].wait_recv()
    gs, us = rF[0, 0].astype(F32), rF[0, 1].astype(F32)
    for t in range(1, nz):
        gs = gs + rF[t, 0].astype(F32)
        us = us + rF[t, 1].astype(F32)
    hG[mt] = (gs / (1.0 + jnp.exp(-gs)) * us).astype(BF16)
    ways, hops = spread(hG, 3)
    for k in range(1, nz):
        dways[k].wait_recv()
        dhops[k].start()

    cdd.wait()
    for cp in edc:
        cp.wait()

    def down(src):
        for e in range(le):
            acc[e] += mm(hG[src, e * slots : (e + 1) * slots], wed[e, aligned(src, fc), :])

    acc[...] = jnp.zeros_like(acc)
    down(mt)
    hops[0].wait_recv()
    down(sib)
    for k in range(1, nz):
        ways[k].wait_recv()
        hops[k].start()
        down(lax.rem(mz + nz - k, nz) * 2 + core)
    for k in range(nz):
        dhops[k].wait_recv()
    dh = hGd[...].astype(F32).reshape(ep * seqs, fd).astype(BF16)
    sH[:, PAD : PAD + seqs] = mm(dh, wdd[...]).astype(BF16).reshape(ep, seqs, own)
    for k in range(1, nz):
        hops[k].wait_recv()
        down(lax.rem(mz + nz - k, nz) * 2 + 1 - core)
    res = acc[...].reshape(nslot, own).astype(BF16)
    back = lax.dot_general(
        perm, res, (((0,), (0,)), ((), ())), preferred_element_type=F32
    ).astype(BF16)
    sH[:, 0:PAD] = back.reshape(ep, PAD, own)
    got = post(10, "ep", lambda p: sH.at[p], lambda m: rH.at[m])
    rH[me] = sH[me]
    arrive(got_mix)
    mixs = mixp[0]
    for t in range(1, tp):
        mixs = mixs + mixp[t]
    gate = 1.0 / (1.0 + jnp.exp(-upright(mixs[0:1])))
    arrive(got)
    returned = rH[:, 0:PAD].reshape(ep * PAD, own)
    hi = mixw.astype(BF16)
    rest = mixw - hi.astype(F32)
    mid = rest.astype(BF16)
    last = (rest - mid.astype(F32)).astype(BF16)
    emix = mm(hi, returned) + mm(mid, returned) + mm(last, returned)
    dout = rH[0, PAD : PAD + seqs].astype(F32)
    for p in range(1, ep):
        dout = dout + rH[p, PAD : PAD + seqs].astype(F32)
    dout = dout.astype(BF16).astype(F32)
    comb = residual_scale * hidf + emix + gate * dout
    s1 = jnp.sum(comb, axis=1, keepdims=True)
    s2 = jnp.sum(comb * comb, axis=1, keepdims=True)
    mom[mt, 0:1] = flat(s1)
    mom[mt, 1:2] = flat(s2)
    got = post(11, "tp", lambda p: mom.at[mt], lambda m: mom.at[m])
    arrive(got)
    ms = mom[0]
    for t in range(1, tp):
        ms = ms + mom[t]
    ms = ms * (1.0 / width)
    avg = upright(ms[0:1])
    var = upright(ms[1:2]) - avg * avg
    out[...] = ((comb - avg) * lax.rsqrt(var + layer_epsilon) * sgain[...]).astype(BF16)

    for cp in sends:
        cp.wait_send()
    for k in range(nz):
        dpair[k].wait_send()
        epair[k].wait_send()
        hops[k].wait_send()
        dhops[k].wait_send()
        if k:
            for cp in (dalong[k], ealong[k], ways[k], dways[k]):
                cp.wait_send()
    for ds in range(ep):
        for h in range(ratio):
            t, cp = dcopy(ds, h)
            if ds == 0:
                @pl.when(t != mt)
                def _():
                    cp.wait_send()
            else:
                cp.wait_send()


PHASES = 12


def on_device(
    tokens, query_weight, key_weight, value_weight, out_weight, head_lambda, head_gain,
    key_cache, value_cache, lengths, first_gain, second_gain, expert_ids, route_weights,
    expert_gate, expert_up, expert_down, dense_gate, dense_up, dense_down, dense_mix,
):
    ep, tp = lax.axis_size("ep"), lax.axis_size("tp")
    seqs, width = tokens.shape
    cache, kv, vd = key_cache.shape[1:]
    heads = head_lambda.shape[0]
    cdim, qc = query_weight.shape
    kcn = key_weight.shape[1]
    le, own, ffe = expert_gate.shape
    fd = dense_gate.shape[1]
    fc = ffe // tp
    ratio = tp // ep
    slots = ep * CAP
    rows = ep * seqs
    npos = cache * kv
    vm = pl.BlockSpec(memory_space=pltpu.VMEM)
    sm = pl.BlockSpec(memory_space=pltpu.SMEM)
    hb = pl.BlockSpec(memory_space=pl.ANY)
    V = pltpu.VMEM
    D = pltpu.SemaphoreType.DMA
    n = max(ep, tp)
    nz = tp // 2
    return pl.pallas_call(
        functools.partial(kernel, ep, tp, kv, heads),
        out_shape=jax.ShapeDtypeStruct((seqs, own), BF16),
        in_specs=[vm, sm, sm] + [vm] * 6 + [hb] * 12,
        out_specs=vm,
        scratch_shapes=[
            V(query_weight.shape, BF16), V(key_weight.shape, BF16), V(value_weight.shape, BF16),
            V(out_weight.shape, BF16),
            V((seqs, npos, vd), BF16), V((seqs, npos, vd), BF16),
            V(expert_gate.shape, BF16), V(expert_up.shape, BF16), V(expert_down.shape, BF16),
            V(dense_gate.shape, BF16), V(dense_up.shape, BF16), V(dense_down.shape, BF16),
            V((ep, seqs, cdim), BF16),
            V((ep, seqs, qc + 2 * kcn), BF16), V((ep, seqs, qc + 2 * kcn), BF16),
            V((seqs, 2 * heads, LANES), F32), V((seqs, 2 * heads, LANES), F32),
            V((seqs, heads, LANES), F32), V((seqs, heads, LANES), F32),
            V((ep, seqs, heads * LANES), BF16),
            V((ratio, ep, seqs, own), BF16), V((tp, seqs, own), BF16),
            V((tp, 2, LANES), F32), V((tp, 2, LANES), F32),
            V((ep, seqs + PAD, own), BF16), V((ep, seqs + PAD, own), BF16),
            V((le * slots, own), BF16),
            V((nz, 2, le * slots, fc), BF16), V((nz, 2, le * slots, fc), BF16),
            V((nz, 2, le * slots, fc), BF16), V((nz, 2, le * slots, fc), BF16),
            V((tp, rows // tp, 2 * fd), BF16), V((nz, rows // tp, 2 * fd), BF16),
            V((nz, rows // tp, 2 * fd), BF16), V((nz, rows // tp, 2 * fd), BF16),
            V((tp, le * slots, fc), BF16), V((tp, rows // tp, fd), BF16),
            V((le, slots, own), F32),
            V((ep, PAD + seqs, own), BF16), V((ep, PAD + seqs, own), BF16),
            V((tp, 2, LANES), F32),
            D((7,)), D((seqs,)), D((seqs,)), D((3, le)),
            D((PHASES, n)), D((PHASES, n)), D((ep, ratio)), D((tp,)),
            D((2, 4, nz)), D((2, 4, nz)),
        ],
        compiler_params=pltpu.CompilerParams(
            collective_id=0, has_side_effects=True, vmem_limit_bytes=62 * 1024 * 1024
        ),
        name="layer",
    )(
        tokens, lengths, head_lambda, head_gain.reshape(1, -1),
        first_gain.reshape(1, -1), second_gain.reshape(1, -1), expert_ids.T, route_weights.T,
        dense_mix.reshape(-1, LANES),
        query_weight, key_weight, value_weight, out_weight,
        key_cache.reshape(seqs, npos, vd), value_cache.reshape(seqs, npos, vd),
        expert_gate, expert_up, expert_down, dense_gate, dense_up, dense_down,
    )


def solution(mesh):
    return jax.shard_map(
        on_device,
        mesh=mesh,
        in_specs=(
            P("ep", None), P("ep", "tp"), P("ep", "tp"), P("ep", "tp"), P("tp", "ep"),
            P("tp"), P(), P("ep", None, "tp", None), P("ep", None, "tp", None), P("ep"),
            P(), P("tp"), P("ep", None), P("ep", None), P("ep", "tp", None),
            P("ep", "tp", None), P("ep", None, "tp"), P("tp", "ep"), P("tp", "ep"),
            P("ep", "tp"), P(),
        ),
        out_specs=P("ep", "tp"),
        check_vma=False,
    )
```
